32 devices in a mesh: grp: 2 (over x), ep: 16 (over z, y, core).
Axes of the slice: x: 2, y: 2, z: 4, core: 2. Of those that a mesh axis runs over, the one named last changes fastest.
Arguments:
- tokens: bfloat16 [1024, 2048], P(('grp', 'ep')), parts along dimension 0, may hold values from -6 to 6
- routes: int32 [1024, 4], P(('grp', 'ep')), parts along dimension 0, may hold values from 0 to 15, all different within a row; in each aligned block of 32 rows (0 to 31, 32 to 63, ...) at most 16 rows name the same one
- in_gain: float32 [2048], replicated, may hold values from 0.1 to 1.9
- group_router: float32 [2048, 4], replicated, may hold values from -0.03125 to 0.03125
- expert_router: float32 [2048, 16], replicated, may hold values from -0.03125 to 0.03125
- w_gate: bfloat16 [16, 2048, 512], P('ep'), may hold values from -0.125 to 0.125
- w_up: bfloat16 [16, 2048, 512], P('ep'), may hold values from -0.125 to 0.125
- w_down: bfloat16 [16, 512, 2048], P('ep')
- out_gain: float32 [2048], P('ep'), may hold values from 0.1 to 1.9
Outputs:
- mixed_out: bfloat16 [1024, 2048], P('grp', 'ep'), parts along dimension 0
The draws below stay inside these ranges and needn't reach their ends.
There are 2 independent parts, one for each index of `grp`. The reference program is written for one: setup_inputs(seed, part) draws one part's arguments, and reference() takes and returns one part's arrays. A program takes and returns all parts, laid end to end along the dimension named above; an argument that names none is the same for every part. Nothing has to cross between parts.
Inputs may be any that keep to these rules, and one draw needn't show every extreme that they name: `routes`: each row names 4 different experts; in the rows of one device no expert is named more than 16 times, a bound that some block reaches.
All inputs are finite; a program needn't handle non-finite values.
Results may differ from the reference program's by a relative error of at most 0.0085.
Values may be sent and summed in bfloat16 or wider, within the bound.
No kernel may reach another device: no remote copies, remote signals or barrier semaphores. Data moves between devices by JAX's collectives and lax.ppermute only.
A program may use at most 64 MiB of HBM per device.

```python
import math
import jax
import jax.numpy as jnp
import numpy as np
from jax import lax

D = 2048
FF = 512
N_GROUPS = 4
TOPK = 4
TOK_DEV = 32
EXPERTS = 16
TOKENS = 512
CAP = 16
N_EP = 16


def draw_w_down(key, part):
    first, second = jax.random.split(jax.random.fold_in(key, 7))
    column = jnp.arange(D, dtype=jnp.float32) / D
    base = jax.random.normal(first, (EXPERTS, FF, D), jnp.float32)
    rising = (1.0 + 2.0 * column) ** 0.5
    rough = jax.random.uniform(second, (D,), jnp.float32, 0.6, 1.4)
    return (base * FF ** (-0.5) * rising * rough).astype(jnp.bfloat16)


def block_scale(stream_key, shape, cuts, smallest, top_value):
    gain, own = 1.0, jax.random.fold_in(stream_key, 6)
    for axis_at, shards_of in cuts:
        steps = jnp.exp(jax.random.uniform(jax.random.fold_in(own, axis_at), (shards_of,), jnp.float32, smallest / len(cuts), top_value / len(cuts)))
        gain = gain * jnp.repeat(steps, shape[axis_at] // shards_of).reshape([-1 if axis == axis_at else 1 for axis in range(len(shape))])
    return gain


def shared_out(key, own, number, rows, count, top, bound, slope):
    order = jax.random.permutation(key, count)
    packed, usual = portions_of(count, rows * top, bound, slope, True), portions_of(count, rows * top, bound, slope, False)
    places = jnp.arange(count)

    def named(lengths, offset_by):
        used = int((lengths > 0).sum())
        fixed = max(1, used // 4)
        shifted = fixed + (places - fixed + offset_by * (used - fixed)) % max(1, count - fixed)
        return jnp.zeros((count,), jnp.int32).at[order[jnp.where(places < fixed, places, shifted)]].set(jnp.asarray(lengths, jnp.int32))

    lengths = jnp.where(number % 4 == 0, named(packed, number // 4), named(usual, number - number // 4 - 1))
    mixed = jax.random.permutation(jax.random.fold_in(own, 3), count)
    source_of, sink = mixed[0:count // 2 * 2:2], mixed[1:count // 2 * 2:2]
    room = jnp.minimum(lengths[source_of] - 1, bound - lengths[sink]) // 2
    room = jnp.where((source_of == order[0]) | (sink == order[0]) | (lengths[sink] == 0), 0, jnp.maximum(room, 0))
    shifted = jax.random.randint(jax.random.fold_in(own, 4), (count // 2,), 0, 1 << 20) % (room + 1)
    lengths = lengths.at[source_of].add(-shifted).at[sink].add(shifted)
    items = jnp.searchsorted(jnp.cumsum(lengths), jnp.arange(rows * top), side="right").astype(jnp.int32)
    table = items.reshape(top, rows).T
    table = table[jax.random.permutation(jax.random.fold_in(own, 1), rows)]
    offset_by = jax.random.randint(jax.random.fold_in(own, 2), (rows, 1), 0, top)
    return jnp.take_along_axis(table, (jnp.arange(top)[None, :] + offset_by) % top, axis=1)


def portions_of(number_of, total, reach, skew, full):
    loads = [(1 << 20) // math.isqrt(grade ** skew) + 1 for grade in range(1, number_of + 1)]
    largest = reach if full else min(reach, max(-(-total // number_of), total * loads[0] // sum(loads)))
    least = 1 if total - largest >= number_of - 1 else 0
    holding, surplus = [largest] + [least] * (number_of - 1), total - largest - least * (number_of - 1)
    while surplus > 0:
        movable = [i for i in range(1, number_of) if holding[i] < largest] or [i for i in range(1, number_of) if holding[i] < reach]
        mass, budget = sum([loads[i] for i in movable]), surplus
        for i in movable:
            addition = min(reach - holding[i], max(1, budget * loads[i] // mass), surplus)
            holding[i] = holding[i] + addition
            surplus = surplus - addition
    return np.array(holding)


def bell_draw(rng, shape, deviation, most, pieces=(), kind=jnp.bfloat16):
    level = block_scale(rng, shape, pieces, -0.22, 0.18) if pieces else 1.0
    array = jax.random.normal(rng, shape, jnp.float32) * deviation * level
    return jnp.minimum(jnp.maximum(array, -most), most).astype(kind)


def setup_inputs(seed: int = 0, part: int = 0) -> dict:
    key_of = jax.random.split(jax.random.key(seed), 10)
    part_splits = jax.random.split(jax.random.fold_in(key_of[9], part), 10)
    tokens = bell_draw(part_splits[0], (TOKENS, D), 1.0, 6.0, ((0, 16),))
    routes_keys = jax.random.split(jax.random.fold_in(part_splits[1], 1), TOKENS // TOK_DEV)
    routes_turns = jax.random.permutation(jax.random.fold_in(part_splits[1], 3), TOKENS // TOK_DEV)
    routes = jax.vmap(lambda own, number: shared_out(jax.random.fold_in(part_splits[1], 2), own, number, TOK_DEV, EXPERTS, TOPK, CAP, 2))(routes_keys, routes_turns).reshape((TOKENS, TOPK))
    in_gain = jnp.clip(1.0 + 0.18 * jax.random.normal(key_of[2], (D,), jnp.float32), 0.1, 1.9)
    group_router = bell_draw(key_of[3], (D, N_GROUPS), (16 * D) ** -0.5, 0.03125, (), jnp.float32)
    expert_router = bell_draw(key_of[4], (D, EXPERTS), (16 * D) ** -0.5, 0.03125, (), jnp.float32)
    w_gate = bell_draw(key_of[5], (EXPERTS, D, FF), D ** -0.5, 0.125, ((0, 16),))
    w_up = bell_draw(key_of[6], (EXPERTS, D, FF), D ** -0.5, 0.125, ((0, 16),))
    w_down = draw_w_down(jax.random.fold_in(key_of[9], 71), part)
    out_gain = jnp.clip(1.0 + 0.18 * jax.random.normal(key_of[8], (D,), jnp.float32), 0.1, 1.9)
    return {"tokens": tokens, "routes": routes, "in_gain": in_gain, "group_router": group_router, "expert_router": expert_router, "w_gate": w_gate, "w_up": w_up, "w_down": w_down, "out_gain": out_gain}


EPSILON = 1e-06

def expert_rows(rows, gate_mat, up_mat, down_mat):
    gate = jnp.dot(rows, gate_mat, preferred_element_type=jnp.float32)
    upward = jnp.dot(rows, up_mat, preferred_element_type=jnp.float32)
    hidden = (jax.nn.silu(gate) * upward).astype(jnp.bfloat16)
    return jnp.dot(hidden, down_mat, preferred_element_type=jnp.float32).astype(jnp.bfloat16)

def reference(tokens, routes, in_gain, group_router, expert_router, w_gate, w_up, w_down, out_gain):
    values = tokens.astype(jnp.float32)
    normed = (values * lax.rsqrt(lax.optimization_barrier(jnp.mean(values * values, axis=1, keepdims=True)) + EPSILON) * in_gain).astype(jnp.bfloat16)
    wide = normed.astype(jnp.float32)
    group_logit = jnp.dot(wide, group_router, precision=lax.Precision.HIGHEST)
    expert_logit = jnp.dot(wide, expert_router, precision=lax.Precision.HIGHEST)
    group_prob = jnp.exp(group_logit) / lax.optimization_barrier(jnp.sum(jnp.exp(group_logit), axis=1, keepdims=True))
    chosen = jnp.exp(jnp.take_along_axis(expert_logit, routes, axis=1))
    expert_prob = chosen / lax.optimization_barrier(jnp.sum(chosen, axis=1, keepdims=True))
    per_group = EXPERTS // N_GROUPS
    weight = jnp.take_along_axis(group_prob, routes // per_group, axis=1) * expert_prob
    pairs = routes.reshape(N_EP, TOK_DEV * TOPK)
    onehot = (pairs[:, :, None] == jnp.arange(EXPERTS, dtype=jnp.int32)).astype(jnp.int32)
    order_in = lax.optimization_barrier(jnp.sum(onehot * (jnp.cumsum(onehot, axis=1) - 1), axis=2)).astype(jnp.int32)
    slot_index = (jnp.arange(N_EP, dtype=jnp.int32)[:, None] * CAP + order_in).reshape(-1)
    expert_of = routes.reshape(-1)
    token_index = jnp.arange(TOKENS * TOPK, dtype=jnp.int32) // TOPK
    table = jnp.zeros((EXPERTS, N_EP * CAP), jnp.int32).at[expert_of, slot_index].set(token_index)
    answers = lax.map(lambda group: expert_rows(normed[group[0]], group[1], group[2], group[3]), (table, w_gate, w_up, w_down))
    pair_rows = answers[expert_of, slot_index].astype(jnp.float32)
    mixed = lax.optimization_barrier(jnp.sum((pair_rows * weight.reshape(-1)[:, None]).reshape(TOKENS, TOPK, D), axis=1))
    scale = lax.rsqrt(lax.optimization_barrier(jnp.mean(mixed * mixed, axis=1, keepdims=True)) + EPSILON)
    return (mixed * scale * out_gain).astype(jnp.bfloat16)
```

```python
import jax
import jax.numpy as jnp
from jax import lax
from jax.experimental import pallas as pl
from jax.experimental.pallas import tpu as pltpu
from jax.sharding import PartitionSpec as P

EPSILON = 1e-06
LANES = 128
F32 = jnp.float32
BF16 = jnp.bfloat16
NT = (((1,), (1,)), ((), ()))


def whole(count, memory=pltpu.VMEM):
    return [pl.BlockSpec(memory_space=memory)] * count


def payload_kernel(tokens, routes, in_gain, group_t, expert_t, out):
    values = tokens[...].astype(F32)
    width = values.shape[1]
    scaled = values * lax.rsqrt(jnp.mean(values * values, axis=1, keepdims=True) + EPSILON)
    normed = (scaled * in_gain[...]).astype(BF16)
    out[:, :width] = normed
    wide = normed.astype(F32)
    dot = lambda router: lax.dot_general(
        wide, router[...], NT, precision=lax.Precision.HIGHEST, preferred_element_type=F32
    )
    group_exp = jnp.exp(dot(group_t))
    expert_exp = jnp.exp(dot(expert_t))
    groups, experts = group_exp.shape[1], expert_exp.shape[1]
    group_prob = group_exp / jnp.sum(group_exp, axis=1, keepdims=True)
    lane = lax.broadcasted_iota(jnp.int32, expert_exp.shape, 1)
    chosen = jnp.zeros(expert_exp.shape, F32)
    for slot in range(routes.shape[1]):
        chosen = jnp.where(routes[:, slot : slot + 1] == lane, expert_exp, chosen)
    spread = jnp.zeros(expert_exp.shape, F32)
    for group in range(groups):
        spread = jnp.where(
            lane // (experts // groups) == group, group_prob[:, group : group + 1], spread
        )
    weight = spread * (chosen / jnp.sum(chosen, axis=1, keepdims=True))
    high = weight.astype(BF16)
    low = (weight - high.astype(F32)).astype(BF16)
    extra = out.shape[1] - width
    row = lax.broadcasted_iota(jnp.int32, (experts, extra), 0)
    column = lax.broadcasted_iota(jnp.int32, (experts, extra), 1)
    place = lambda shift: jnp.where(column == row + shift, 1.0, 0.0).astype(BF16)
    ext = jnp.dot(high, place(0), preferred_element_type=F32)
    ext = ext + jnp.dot(low, place(experts), preferred_element_type=F32)
    out[:, width:] = ext.astype(BF16)


def expert_body(far, width, experts, block):
    def kernel(where_at, *refs):
        near_refs, peer_refs = refs[:far], refs[far : 2 * far]
        w_gate, w_up, w_down = refs[2 * far : 2 * far + 3]
        keep, send = refs[2 * far + 3 : 3 * far + 3], refs[3 * far + 3 : 4 * far + 3]
        rows, result = refs[4 * far + 3], refs[4 * far + 4]
        mine = where_at[0]
        top, mid, low = mine // 4, (mine // 2) % 2, mine % 2
        tok = near_refs[0].shape[1]
        for q in range(far):
            for s in range(2):
                base = ((top + far - q) % far) * 4 + (mid ^ s) * 2
                for r, ref in ((0, near_refs[q]), (1, peer_refs[q])):
                    at = pl.multiple_of((base + (low ^ r)) * tok, tok)
                    rows[pl.ds(at, tok), :] = ref[s]
        ext = rows[:, width:].astype(F32)
        lane = lax.broadcasted_iota(jnp.int32, ext.shape, 1)
        hit = (lane == mine) | (lane == mine + experts)
        weight = jnp.sum(jnp.where(hit, ext, 0.0), axis=1, keepdims=True)
        data = rows[:, :width]
        gate = jnp.dot(data, w_gate[0], preferred_element_type=F32)
        upward = jnp.dot(data, w_up[0], preferred_element_type=F32)
        hidden = (gate / (1.0 + jnp.exp(-gate)) * upward * weight).astype(BF16)
        result[...] = jnp.dot(hidden, w_down[0], preferred_element_type=F32).astype(BF16)
        for q in range(far):
            for s in range(2):
                at = (((top + q) % far) * 2 + (mid ^ s)) * 2 * block
                pair = result[:, pl.ds(pl.multiple_of(at, 2 * block), 2 * block)]
                left, right = pair[:, :block], pair[:, block:]
                keep[q][s] = jnp.where(low == 0, left, right)
                send[q][s] = jnp.where(low == 0, right, left)

    return kernel


def add(one, two):
    return (one.astype(F32) + two.astype(F32)).astype(BF16)


def per_device(
    tokens, routes, in_gain, group_router, expert_router, w_gate, w_up, w_down, out_gain
):
    tok, width = tokens.shape
    experts = expert_router.shape[1]
    ep = lax.axis_size("ep")
    far, block = ep // 4, width // ep
    extra = -(-2 * experts // LANES) * LANES
    mine = lax.axis_index("ep").astype(jnp.int32)

    def flip(value, bit):
        return lax.ppermute(value, "ep", [(i, i ^ bit) for i in range(ep)])

    def shift(value, step):
        moves = [(i, ((i // 4 + step) % far) * 4 + i % 4) for i in range(ep)]
        return lax.ppermute(value, "ep", moves)

    payload = pl.pallas_call(
        payload_kernel,
        out_shape=jax.ShapeDtypeStruct((tok, width + extra), BF16),
        in_specs=whole(5),
        out_specs=pl.BlockSpec(memory_space=pltpu.VMEM),
    )(tokens, routes, in_gain[None, :], group_router.T, expert_router.T)

    steps = [1, far - 1] + [q for q in range(2, far - 1)]
    held = {0: payload}
    for q in steps:
        held[q] = shift(payload, q)
    near, peer = {}, {}
    for q in [0] + steps:
        near[q] = jnp.stack([held[q], flip(held[q], 2)])
        peer[q] = flip(near[q], 1)
    total = ep * tok
    piece = jax.ShapeDtypeStruct((2, total, block), BF16)
    parts = pl.pallas_call(
        expert_body(far, width, experts, block),
        out_shape=[piece] * (2 * far),
        in_specs=whole(1, pltpu.SMEM) + whole(2 * far + 3),
        out_specs=whole(2 * far),
        scratch_shapes=[
            pltpu.VMEM((total, width + extra), BF16),
            pltpu.VMEM((total, width), BF16),
        ],
    )(
        mine[None],
        *[near[q] for q in range(far)],
        *[peer[q] for q in range(far)],
        w_gate,
        w_up,
        w_down,
    )
    keep, send = parts[:far], parts[far:]
    order = [q for q in range(2, far - 1)] + [1, far - 1, 0]
    landed = {}
    for q in order:
        paired = add(keep[q], flip(send[q], 1))
        squared = add(paired[0], flip(paired[1], 2))
        landed[q] = shift(squared, q) if q else squared
    mixed = landed[0].astype(F32)
    for q in order[:-1]:
        mixed = mixed + landed[q].astype(F32)
    power = jnp.sum(mixed * mixed, axis=1)
    power = power + flip(power, 1)
    power = power + flip(power, 2)
    others = [shift(power, q) for q in range(1, far)]
    for other in others:
        power = power + other
    scale = lax.rsqrt(power / width + EPSILON)
    return (mixed * scale[:, None] * out_gain).astype(BF16)


def solution(mesh):
    in_specs = (
        P(("grp", "ep"), None),
        P(("grp", "ep"), None),
        P(),
        P(),
        P(),
        P("ep", None, None),
        P("ep", None, None),
        P("ep", None, None),
        P("ep"),
    )
    out_specs = P("grp", "ep")
    return jax.shard_map(
        per_device, mesh=mesh, in_specs=in_specs, out_specs=out_specs, check_vma=False
    )
```

```python
import jax
import jax.numpy as jnp
from jax import lax
from jax.experimental import pallas as pl
from jax.experimental.pallas import tpu as pltpu
from jax.sharding import PartitionSpec as P


EPSILON = 1e-06
LANES = 128
F32 = jnp.float32
BF16 = jnp.bfloat16
NT = (((1,), (1,)), ((), ()))
TN = (((0,), (0,)), ((), ()))


def whole(count, memory=pltpu.VMEM):
    return [pl.BlockSpec(memory_space=memory)] * count


def payload_kernel(tokens, routes, in_gain, group_t, expert_t, out):
    values = tokens[...].astype(F32)
    width = values.shape[1]
    scaled = values * lax.rsqrt(jnp.mean(values * values, axis=1, keepdims=True) + EPSILON)
    normed = (scaled * in_gain[...]).astype(BF16)
    out[:, :width] = normed
    wide = normed.astype(F32)
    dot = lambda router: lax.dot_general(
        router[...], wide, NT, precision=lax.Precision.HIGHEST, preferred_element_type=F32
    )
    group_exp = jnp.exp(dot(group_t))
    expert_exp = jnp.exp(dot(expert_t))
    groups, experts = group_exp.shape[0], expert_exp.shape[0]
    group_prob = group_exp / jnp.sum(group_exp, axis=0, keepdims=True)
    lane = lax.broadcasted_iota(jnp.int32, expert_exp.shape, 0)
    chosen = jnp.zeros(expert_exp.shape, F32)
    for slot in range(routes.shape[0]):
        chosen = jnp.where(routes[slot : slot + 1, :] == lane, expert_exp, chosen)
    spread = jnp.zeros(expert_exp.shape, F32)
    for group in range(groups):
        spread = jnp.where(
            lane // (experts // groups) == group, group_prob[group : group + 1, :], spread
        )
    weight = spread * (chosen / jnp.sum(chosen, axis=0, keepdims=True))
    high = weight.astype(BF16)
    low = (weight - high.astype(F32)).astype(BF16)
    extra = out.shape[1] - width
    row = lax.broadcasted_iota(jnp.int32, (experts, extra), 0)
    column = lax.broadcasted_iota(jnp.int32, (experts, extra), 1)
    place = lambda move: jnp.where(column == row + move, 1.0, 0.0).astype(BF16)
    spot = lambda part, move: lax.dot_general(
        part, place(move), TN, preferred_element_type=F32
    )
    ext = spot(high, 0) + spot(low, experts)
    out[:, width:] = ext.astype(BF16)


def expert_body(far, width, experts, block):
    def kernel(where_at, *refs):
        near_refs, peer_refs = refs[:far], refs[far : 2 * far]
        w_gate, up_far, down_far = refs[2 * far : 2 * far + 3]
        keep, send = refs[2 * far + 3 : 3 * far + 3], refs[3 * far + 3 : 4 * far + 3]
        rows, result, w_up, w_down, up_done, down_done = refs[4 * far + 3 :]
        up_copy = pltpu.make_async_copy(up_far, w_up, up_done)
        down_copy = pltpu.make_async_copy(down_far, w_down, down_done)
        up_copy.start()
        down_copy.start()
        mine = where_at[0]
        top, mid, low = mine // 4, (mine // 2) % 2, mine % 2
        tok = near_refs[0].shape[1]
        for q in range(far):
            for s in range(2):
                base = ((top + far - q) % far) * 4 + (mid ^ s) * 2
                for r, ref in ((0, near_refs[q]), (1, peer_refs[q])):
                    at = pl.multiple_of((base + (low ^ r)) * tok, tok)
                    rows[pl.ds(at, tok), :] = ref[s]
        ext = rows[:, width:].astype(F32)
        lane = lax.broadcasted_iota(jnp.int32, ext.shape, 1)
        hit = (lane == mine) | (lane == mine + experts)
        weight = jnp.sum(jnp.where(hit, ext, 0.0), axis=1, keepdims=True)
        data = rows[:, :width]
        gate = jnp.dot(data, w_gate[0], preferred_element_type=F32)
        up_copy.wait()
        upward = jnp.dot(data, w_up[0], preferred_element_type=F32)
        hidden = (gate / (1.0 + jnp.exp(-gate)) * upward * weight).astype(BF16)
        down_copy.wait()
        result[...] = jnp.dot(hidden, w_down[0], preferred_element_type=F32).astype(BF16)
        for q in range(far):
            for s in range(2):
                at = (((top + q) % far) * 2 + (mid ^ s)) * 2 * block
                pair = result[:, pl.ds(pl.multiple_of(at, 2 * block), 2 * block)]
                left, right = pair[:, :block], pair[:, block:]
                keep[q][s] = jnp.where(low == 0, left, right)
                send[q][s] = jnp.where(low == 0, right, left)

    return kernel


def add(one, two):
    return (one.astype(F32) + two.astype(F32)).astype(BF16)


def far_order(far):
    return sorted(range(1, far), key=lambda q: -min(q, far - q))


def per_device(
    tokens, routes, in_gain, group_router, expert_router, w_gate, w_up, w_down, out_gain
):
    tok, width = tokens.shape
    experts = expert_router.shape[1]
    ep = lax.axis_size("ep")
    far, block = ep // 4, width // ep
    extra = -(-2 * experts // LANES) * LANES
    mine = lax.axis_index("ep").astype(jnp.int32)

    def flip(value, bit):
        return lax.ppermute(value, "ep", [(i, i ^ bit) for i in range(ep)])

    def shift(value, step):
        moves = [(i, ((i // 4 + step) % far) * 4 + i % 4) for i in range(ep)]
        return lax.ppermute(value, "ep", moves)

    payload = pl.pallas_call(
        payload_kernel,
        out_shape=pltpu.VMEM((tok, width + extra), BF16),
        in_specs=whole(5),
        out_specs=pl.BlockSpec(memory_space=pltpu.VMEM),
    )(tokens, routes.T, in_gain[None, :], group_router.T, expert_router.T)

    steps = far_order(far)
    held = {0: payload}
    for q in steps:
        held[q] = shift(payload, q)
    near, peer = {}, {}
    for q in [0] + steps:
        near[q] = jnp.stack([held[q], flip(held[q], 2)])
        peer[q] = flip(near[q], 1)
    total = ep * tok
    piece = pltpu.VMEM((2, total, block), BF16)
    local = lambda value: pltpu.with_memory_space_constraint(value, pltpu.VMEM)
    parts = pl.pallas_call(
        expert_body(far, width, experts, block),
        out_shape=[piece] * (2 * far),
        in_specs=whole(1, pltpu.SMEM) + whole(2 * far + 1) + whole(2, pltpu.HBM),
        out_specs=whole(2 * far),
        scratch_shapes=[
            pltpu.VMEM((total, width + extra), BF16),
            pltpu.VMEM((total, width), BF16),
            pltpu.VMEM(w_up.shape, BF16),
            pltpu.VMEM(w_down.shape, BF16),
            pltpu.SemaphoreType.DMA,
            pltpu.SemaphoreType.DMA,
        ],
        compiler_params=pltpu.CompilerParams(vmem_limit_bytes=28 << 20),
    )(
        mine[None],
        *[local(near[q]) for q in range(far)],
        *[local(peer[q]) for q in range(far)],
        local(w_gate),
        pltpu.with_memory_space_constraint(w_up, pltpu.HBM),
        pltpu.with_memory_space_constraint(w_down, pltpu.HBM),
    )
    keep, send = parts[:far], parts[far:]
    order = steps + [0]
    landed = {}
    for q in order:
        paired = add(keep[q], flip(send[q], 1))
        squared = add(paired[0], flip(paired[1], 2))
        landed[q] = shift(squared, q) if q else squared
    mixed = landed[0].astype(F32)
    for q in order[:-1]:
        mixed = mixed + landed[q].astype(F32)
    power = jnp.sum(mixed * mixed, axis=1)
    power = power + flip(power, 1)
    power = power + flip(power, 2)
    others = [shift(power, q) for q in range(1, far)]
    for other in others:
        power = power + other
    scale = lax.rsqrt(power / width + EPSILON)
    return (mixed * scale[:, None] * out_gain).astype(BF16)


def solution(mesh):
    in_specs = (
        P(("grp", "ep"), None),
        P(("grp", "ep"), None),
        P(),
        P(),
        P(),
        P("ep", None, None),
        P("ep", None, None),
        P("ep", None, None),
        P("ep"),
    )
    out_specs = P("grp", "ep")
    return jax.shard_map(
        per_device, mesh=mesh, in_specs=in_specs, out_specs=out_specs, check_vma=False
    )
```
